32 devices in a mesh: grp: 2 (over y), fs: 4 (over z), tp: 4 (over x, core).
Axes of the slice: x: 2, y: 2, z: 4, core: 2. Of those that a mesh axis runs over, the one named last changes fastest.
Arguments:
- tokens: bfloat16 [8192, 2048], P(('grp', 'fs'), 'tp'), parts along dimension 0, may hold values from -6 to 6
- mixer_gain: float32 [2048], replicated, may hold values from 0.1 to 1.9
- branch_weight: float32 [2048, 1024], P('fs', 'tp'), may hold values from -0.125 to 0.125
- gelu_weight: float32 [2048, 1024], P('fs', 'tp'), may hold values from -0.125 to 0.125
- branch_scale: float32 [4, 256], P('fs', 'tp'), may hold values from 0.5 to 2
- gelu_scale: float32 [4, 256], P('fs', 'tp'), may hold values from 0.5 to 2
- branch_taps: float32 [4, 1024], P(None, 'tp'), may hold values from -3 to 3
- recur_gate: bfloat16 [16, 64, 64], P('tp'), may hold values from -0.75 to 0.75
- input_gate: bfloat16 [16, 64, 64], P('tp'), may hold values from -0.75 to 0.75
- decay_param: float32 [1024], P('tp'), may hold values from 4 to 7
- out_weight: float32 [1024, 2048], P('tp', 'fs'), may hold values from -0.5 to 0.5
- out_scale: float32 [4, 512], P('fs'), may hold values from 0.5 to 2
- ffn_gain: float32 [2048], replicated, may hold values from 0.1 to 1.9
- upgate_weight: float32 [2048, 5632], P('fs', 'tp'), may hold values from -0.125 to 0.125
- upval_weight: float32 [2048, 5632], P('fs', 'tp'), may hold values from -0.125 to 0.125
- upgate_scale: float32 [4, 1408], P('fs', 'tp'), may hold values from 0.5 to 2
- upval_scale: float32 [4, 1408], P('fs', 'tp'), may hold values from 0.5 to 2
- upgate_taps: float32 [3, 5632], P(None, 'tp'), may hold values from -3 to 3
- upval_taps: float32 [3, 5632], P(None, 'tp'), may hold values from -3 to 3
- down_weight: float32 [5632, 2048], P('tp', 'fs'), may hold values from -0.15625 to 0.15625
- down_scale: float32 [4, 512], P('fs'), may hold values from 0.5 to 2
Outputs:
- layer_out: bfloat16 [8192, 2048], P(('grp', 'fs'), 'tp'), parts along dimension 0
The draws below stay inside these ranges and needn't reach their ends.
There are 2 independent parts, one for each index of `grp`. The reference program is written for one: setup_inputs(seed, part) draws one part's arguments, and reference() takes and returns one part's arrays. A program takes and returns all parts, laid end to end along the dimension named above; an argument that names none is the same for every part. Nothing has to cross between parts.
All inputs are finite; a program needn't handle non-finite values.
Results may differ from the reference program's by a relative error of at most 0.024.
Values may be sent and summed in bfloat16 or wider, within the bound.
A program may use at most 128 MiB of HBM per device.

```python
import math
import jax
import jax.numpy as jnp
from jax import lax

D = 2048
LRU = 1024
LRU_BLOCK = 64
NB = 16
CONV_LRU = 4
FF = 5632
CONV_FF = 3
SEQ_LEN = 512
TOKENS = 4096
N_FS = 4
N_TP = 4


def draw_decay_param(key, part):
    pick_key, slow_key, fast_key = jax.random.split(jax.random.fold_in(key, 11), 3)
    share = 0.5
    chooser = jax.random.uniform(pick_key, (LRU,), jnp.float32)
    slow_vals = jax.random.uniform(slow_key, (LRU,), jnp.float32, 6.0, 7.0)
    fast_vals = jax.random.uniform(fast_key, (LRU,), jnp.float32, 4.0, 5.0)
    return jnp.where(chooser < share, slow_vals, fast_vals).astype(jnp.float32)


def shard_levels(own_key, shape, pieces, smallest, high):
    level, own = 1.0, jax.random.fold_in(own_key, 6)
    for position, blocks in pieces:
        steps = jnp.exp(jax.random.uniform(jax.random.fold_in(own, position), (blocks,), jnp.float32, smallest / len(pieces), high / len(pieces)))
        level = level * jnp.repeat(steps, shape[position] // blocks).reshape([-1 if axis == position else 1 for axis in range(len(shape))])
    return level


def centred(stream_key, dims, scale, limit, shards=(), kind=jnp.bfloat16):
    entries = jax.random.normal(stream_key, dims, jnp.float32) * scale
    if len(shards) > 0:
        entries = shard_levels(stream_key, dims, shards, -0.22, 0.18) * entries
    return jnp.clip(entries, min=-limit, max=limit).astype(kind)


def setup_inputs(seed: int = 0, part: int = 0) -> dict:
    streams_of = jax.random.split(jax.random.key(seed), 22)
    own_keys = jax.random.split(jax.random.fold_in(streams_of[21], part), 22)
    return {
        "tokens": centred(own_keys[0], (TOKENS, D), 1.0, 6.0, ((0, 4), (1, 4))),
        "mixer_gain": jnp.clip(1.0 + 0.18 * jax.random.normal(streams_of[1], (D,), jnp.float32), 0.1, 1.9),
        "branch_weight": centred(streams_of[2], (D, LRU), D ** -0.5, 0.125, ((0, 4), (1, 4)), jnp.float32),
        "gelu_weight": centred(streams_of[3], (D, LRU), D ** -0.5, 0.125, ((0, 4), (1, 4)), jnp.float32),
        "branch_scale": jnp.clip(jnp.exp(math.log(2.0) - 1.3862944 * jax.random.uniform(streams_of[4], (N_FS, LRU // N_FS), jnp.float32) ** shard_levels(streams_of[4], (N_FS, LRU // N_FS), ((0, 4), (1, 4)), -0.2, 0.2)), 0.5, 2.0),
        "gelu_scale": jnp.clip(jnp.exp(math.log(2.0) - 1.3862944 * jax.random.uniform(streams_of[5], (N_FS, LRU // N_FS), jnp.float32) ** shard_levels(streams_of[5], (N_FS, LRU // N_FS), ((0, 4), (1, 4)), -0.2, 0.2)), 0.5, 2.0),
        "branch_taps": centred(streams_of[6], (CONV_LRU, LRU), 0.5, 3.0, ((1, 4),), jnp.float32),
        "recur_gate": centred(streams_of[7], (NB, LRU_BLOCK, LRU_BLOCK), LRU_BLOCK ** -0.5, 0.75, ((0, 4),)),
        "input_gate": centred(streams_of[8], (NB, LRU_BLOCK, LRU_BLOCK), LRU_BLOCK ** -0.5, 0.75, ((0, 4),)),
        "decay_param": draw_decay_param(jax.random.fold_in(streams_of[21], 71), part),
        "out_weight": centred(streams_of[10], (LRU, D), (LRU // 8) ** -0.5, 0.5, ((0, 4), (1, 4)), jnp.float32),
        "out_scale": jnp.clip(jnp.exp(math.log(2.0) - 1.3862944 * jax.random.uniform(streams_of[11], (N_FS, D // N_FS), jnp.float32) ** shard_levels(streams_of[11], (N_FS, D // N_FS), ((0, 4),), -0.2, 0.2)), 0.5, 2.0),
        "ffn_gain": jnp.clip(1.0 + 0.18 * jax.random.normal(streams_of[12], (D,), jnp.float32), 0.1, 1.9),
        "upgate_weight": centred(streams_of[13], (D, FF), D ** -0.5, 0.125, ((0, 4), (1, 4)), jnp.float32),
        "upval_weight": centred(streams_of[14], (D, FF), D ** -0.5, 0.125, ((0, 4), (1, 4)), jnp.float32),
        "upgate_scale": jnp.clip(jnp.exp(math.log(2.0) - 1.3862944 * jax.random.uniform(streams_of[15], (N_FS, FF // N_FS), jnp.float32) ** shard_levels(streams_of[15], (N_FS, FF // N_FS), ((0, 4), (1, 4)), -0.2, 0.2)), 0.5, 2.0),
        "upval_scale": jnp.clip(jnp.exp(math.log(2.0) - 1.3862944 * jax.random.uniform(streams_of[16], (N_FS, FF // N_FS), jnp.float32) ** shard_levels(streams_of[16], (N_FS, FF // N_FS), ((0, 4), (1, 4)), -0.2, 0.2)), 0.5, 2.0),
        "upgate_taps": centred(streams_of[17], (CONV_FF, FF), 0.577, 3.0, ((1, 4),), jnp.float32),
        "upval_taps": centred(streams_of[18], (CONV_FF, FF), 0.577, 3.0, ((1, 4),), jnp.float32),
        "down_weight": centred(streams_of[19], (FF, D), (FF // 4) ** -0.5, 0.15625, ((0, 4), (1, 4)), jnp.float32),
        "down_scale": jnp.clip(jnp.exp(math.log(2.0) - 1.3862944 * jax.random.uniform(streams_of[20], (N_FS, D // N_FS), jnp.float32) ** shard_levels(streams_of[20], (N_FS, D // N_FS), ((0, 4),), -0.2, 0.2)), 0.5, 2.0),
    }


def rms_rows(values_in, norm_gain):
    values = values_in.astype(jnp.float32)
    inverse = lax.rsqrt(lax.optimization_barrier(jnp.mean(values * values, axis=-1, keepdims=True)) + 1e-06)
    return (values * inverse * norm_gain.astype(jnp.float32)).astype(jnp.bfloat16)

def col_scale(scale_table):
    return scale_table.T.reshape(-1)

def causal_mix(values, filter_taps, seq_len):
    columns = values.shape[-1]
    grouped = values.reshape(-1, seq_len, columns)
    tap_count = filter_taps.shape[0]
    padded = jnp.pad(grouped, ((0, 0), (tap_count - 1, 0), (0, 0)))
    totals = padded[:, 0:seq_len] * filter_taps[0]
    for k in range(1, tap_count):
        totals = totals + padded[:, k:k + seq_len] * filter_taps[k]
    return totals.reshape(-1, columns)

def combine_pairs(earlier, later):
    return (earlier[0] * later[0], later[0] * earlier[1] + later[1])

def run_scan(factors, inputs, seq_len):
    columns = factors.shape[-1]
    pair = (factors.reshape(-1, seq_len, columns), inputs.reshape(-1, seq_len, columns))
    _, states = lax.associative_scan(combine_pairs, pair, axis=1)
    return states.reshape(-1, columns)

def block_sum(left, weight, scales, parts):
    block_rows = left.shape[1] // parts
    totals = jnp.zeros((left.shape[0], weight.shape[1]), jnp.float32)
    for index in range(parts):
        partial_value = jnp.dot(left[:, index * block_rows:(index + 1) * block_rows], weight[index * block_rows:(index + 1) * block_rows], preferred_element_type=jnp.float32) * scales
        totals = totals + lax.optimization_barrier(partial_value.astype(jnp.bfloat16)).astype(jnp.float32)
    return totals

def reference(tokens, mixer_gain, branch_weight, gelu_weight, branch_scale, gelu_scale, branch_taps, recur_gate, input_gate, decay_param, out_weight, out_scale, ffn_gain, upgate_weight, upval_weight, upgate_scale, upval_scale, upgate_taps, upval_taps, down_weight, down_scale):
    normed = rms_rows(tokens, mixer_gain)
    branch = jnp.dot(normed, branch_weight.astype(jnp.bfloat16), preferred_element_type=jnp.float32) * col_scale(branch_scale)
    gelu_in = jnp.dot(normed, gelu_weight.astype(jnp.bfloat16), preferred_element_type=jnp.float32) * col_scale(gelu_scale)
    convolved = causal_mix(branch, branch_taps, SEQ_LEN).astype(jnp.bfloat16)
    blocks = convolved.astype(jnp.float32).reshape(-1, NB, LRU_BLOCK)
    recur = jax.nn.sigmoid(jnp.einsum('rnc,ncd->rnd', blocks, recur_gate.astype(jnp.float32)).reshape(-1, LRU))
    input_rate = jax.nn.sigmoid(jnp.einsum('rnc,ncd->rnd', blocks, input_gate.astype(jnp.float32)).reshape(-1, LRU))
    log_decay = -8.0 * recur * jax.nn.softplus(-decay_param)
    decay_rate = jnp.exp(log_decay)
    driven = jnp.sqrt(-jnp.expm1(2.0 * log_decay)) * input_rate * convolved.astype(jnp.float32)
    states = run_scan(decay_rate, driven, SEQ_LEN)
    gated_state = (states * jax.nn.gelu(gelu_in)).astype(jnp.bfloat16)
    mixer_sum = block_sum(gated_state, out_weight.astype(jnp.bfloat16), col_scale(out_scale), N_TP)
    hidden_state = (tokens.astype(jnp.float32) + mixer_sum).astype(jnp.bfloat16)
    normed_ffn = rms_rows(hidden_state, ffn_gain)
    up_gate = jnp.dot(normed_ffn, upgate_weight.astype(jnp.bfloat16), preferred_element_type=jnp.float32) * col_scale(upgate_scale)
    up_val = jnp.dot(normed_ffn, upval_weight.astype(jnp.bfloat16), preferred_element_type=jnp.float32) * col_scale(upval_scale)
    conv_gate = causal_mix(up_gate, upgate_taps, SEQ_LEN)
    conv_val = causal_mix(up_val, upval_taps, SEQ_LEN)
    ffn_hidden = (jax.nn.silu(conv_gate) * conv_val).astype(jnp.bfloat16)
    ffn_sum = block_sum(ffn_hidden, down_weight.astype(jnp.bfloat16), col_scale(down_scale), N_TP)
    return (hidden_state.astype(jnp.float32) + ffn_sum).astype(jnp.bfloat16)
```

```python
import functools

import jax
import jax.numpy as jnp
from jax import lax
from jax.experimental import pallas as pl
from jax.experimental.pallas import tpu as pltpu
from jax.sharding import PartitionSpec as P

SEQ_LEN = 512
MESH = pl.DeviceIdType.MESH
VMEM = pl.BlockSpec(memory_space=pltpu.VMEM)
CHUNKS = 4


def expand_scale(gathered):
    return gathered.T.reshape(-1)


def causal_mix(values, filter_taps, seq_len):
    columns = values.shape[-1]
    grouped = values.reshape(-1, seq_len, columns)
    tap_count = filter_taps.shape[0]
    padded = jnp.pad(grouped, ((0, 0), (tap_count - 1, 0), (0, 0)))
    totals = padded[:, 0:seq_len] * filter_taps[0]
    for k in range(1, tap_count):
        totals = totals + padded[:, k : k + seq_len] * filter_taps[k]
    return totals.reshape(-1, columns)


def mixer_kernel(branch_ref, gelu_ref, bscale_ref, gscale_ref, taps_ref, rg_ref, ig_ref, sp_ref, out_ref):
    branch = branch_ref[...] * bscale_ref[...]
    rows = branch.shape[0]
    position = lax.broadcasted_iota(jnp.int32, branch.shape, 0)

    def delayed(values, shift, fill):
        return jnp.where(position >= shift, pltpu.roll(values, shift, 0), fill)

    taps = taps_ref.shape[0]
    conv = branch * taps_ref[taps - 1 : taps, :]
    for k in range(taps - 1):
        conv = conv + delayed(branch, taps - 1 - k, 0.0) * taps_ref[k : k + 1, :]
    conv_bf = conv.astype(jnp.bfloat16)
    conv = conv_bf.astype(jnp.float32)
    recur = jax.nn.sigmoid(jnp.dot(conv_bf, rg_ref[...], preferred_element_type=jnp.float32))
    rate = jax.nn.sigmoid(jnp.dot(conv_bf, ig_ref[...], preferred_element_type=jnp.float32))
    log_decay = -8.0 * recur * sp_ref[...]
    factor = jnp.exp(log_decay)
    state = jnp.sqrt(-jnp.tanh(log_decay) * (factor * factor + 1.0)) * rate * conv
    shift = 1
    while shift < rows:
        state = factor * delayed(state, shift, 0.0) + state
        factor = factor * delayed(factor, shift, 1.0)
        shift *= 2
    gelu_in = gelu_ref[...] * gscale_ref[...]
    out_ref[...] = (state * jax.nn.gelu(gelu_in)).astype(jnp.bfloat16)


def block_diagonal(gate, per):
    count, width, _ = gate.shape
    grouped = gate.reshape(count // per, per, width, width)
    eye = jnp.eye(per, dtype=gate.dtype)
    return jnp.einsum("gpab,pq->gpaqb", grouped, eye).reshape(count // per, per * width, per * width)


def mixer(branch, gelu_in, bscale, gscale, taps, recur_gate, input_gate, softplus):
    rows, channels = branch.shape
    lanes = min(channels, 128)
    per = lanes // recur_gate.shape[1]
    rg, ig = block_diagonal(recur_gate, per), block_diagonal(input_gate, per)
    tile = pl.BlockSpec((SEQ_LEN, lanes), lambda s, c: (s, c))
    row = pl.BlockSpec((1, lanes), lambda s, c: (0, c))
    gate = pl.BlockSpec((None, lanes, lanes), lambda s, c: (c, 0, 0))
    return pl.pallas_call(
        mixer_kernel,
        grid=(rows // SEQ_LEN, channels // lanes),
        out_shape=jax.ShapeDtypeStruct((rows, channels), jnp.bfloat16),
        in_specs=[
            tile, tile, row, row,
            pl.BlockSpec((taps.shape[0], lanes), lambda s, c: (0, c)),
            gate, gate, row,
        ],
        out_specs=tile,
        cost_estimate=pl.CostEstimate(flops=10**8, bytes_accessed=10 * rows * channels, transcendentals=rows * channels * 6),
    )(branch, gelu_in, bscale[None], gscale[None], taps, rg, ig, softplus[None])


class Across:
    def __init__(self, tp, src, held, local_sem, pair_sems, sends, recvs, fsends, frecvs):
        self.src, self.held, self.local_sem, self.pair_sems = src, held, local_sem, pair_sems
        self.sems = (sends, recvs, fsends, frecvs)
        self.me = lax.axis_index("tp")
        self.core, self.chips = lax.rem(self.me, 2), tp // 2
        self.chip = self.me // 2
        self.partner = self.me + 1 - 2 * self.core
        self.rows = src.shape[0] // CHUNKS
        self.others = [
            lax.rem(self.chip + d, self.chips) * 2 + self.core for d in range(1, self.chips)]
        self.open = []

    def copy(self, source, dest, send, recv, device):
        return pltpu.make_async_remote_copy(
            src_ref=source, dst_ref=dest, send_sem=send, recv_sem=recv,
            device_id={"tp": device}, device_id_type=MESH)

    def start_part(self, k):
        part = pl.ds(k * self.rows, self.rows)
        for d in range(1, self.chips):
            copy = self.copy(
                self.src.at[part], self.held.at[self.me, part], self.sems[0].at[d - 1, k],
                self.sems[1].at[d - 1, k], self.others[d - 1])
            copy.start()
            self.open.append(copy.wait_send)

    def start_own(self):
        own = pltpu.make_async_copy(self.src, self.held.at[self.me], self.local_sem)
        own.start()
        pair = self.copy(
            self.src, self.held.at[self.me], self.pair_sems.at[0], self.pair_sems.at[1],
            self.partner)
        pair.start()
        self.open += [own.wait, pair.wait]

    def forward(self, k):
        part = pl.ds(k * self.rows, self.rows)
        for d in range(1, self.chips):
            source = lax.rem(self.chip - d + self.chips, self.chips) * 2 + self.core
            self.copy(
                self.src.at[part], self.held.at[source, part], self.sems[0].at[d - 1, k],
                self.sems[1].at[d - 1, k], self.others[d - 1]).wait_recv()
            onward = self.copy(
                self.held.at[source, part], self.held.at[source, part],
                self.sems[2].at[d - 1, k], self.sems[3].at[d - 1, k], self.partner)
            onward.start()
            self.open.append(onward.wait)

    def finish(self):
        for wait in self.open:
            wait()


def across_scratch(tp, rows, columns):
    many = pltpu.SemaphoreType.DMA((tp // 2 - 1, CHUNKS))
    return [
        pltpu.VMEM((tp, rows, columns), jnp.bfloat16),
        pltpu.SemaphoreType.DMA, pltpu.SemaphoreType.DMA((2,)), many, many, many, many,
    ]


class Along:
    def __init__(self, fs, src, out, sems, local_sem):
        self.fs, self.src, self.out, self.sems, self.local_sem = fs, src, out, sems, local_sem
        self.z, self.y = lax.axis_index("fs"), lax.axis_index("grp")

    def cases(self, s):
        z, fs = self.z, self.fs
        return (
            (0, (z >= s - 1) & (z <= fs - 2), z - s + 1, z + 1, z >= s, z - s),
            (1, (z >= 1) & (z <= fs - s), z + s - 1, z - 1, z <= fs - 1 - s, z + s),
        )

    def hop(self, s, way, shard, device):
        source = self.src.at[self.y] if s == 1 else self.out.at[shard, self.y]
        return pltpu.make_async_remote_copy(
            src_ref=source, dst_ref=self.out.at[shard, self.y],
            send_sem=self.sems.at[0, way, s - 1], recv_sem=self.sems.at[1, way, s - 1],
            device_id={"fs": device}, device_id_type=MESH)

    def swap(self, s, way, shard, half):
        where = self.out.at[shard, half]
        return pltpu.make_async_remote_copy(
            src_ref=where, dst_ref=where,
            send_sem=self.sems.at[2, way, s - 1], recv_sem=self.sems.at[3, way, s - 1],
            device_id={"grp": 1 - self.y}, device_id_type=MESH)

    def start(self):
        self.own = pltpu.make_async_copy(self.src, self.out.at[self.z], self.local_sem)
        self.send(1)
        self.own.start()

    def send(self, s):
        for way, sends, shard, device, _, _ in self.cases(s):
            @pl.when(sends)
            def _():
                self.hop(s, way, shard, device).start()

    def pump(self, s):
        for way, _, _, _, gets, shard in self.cases(s):
            @pl.when(gets)
            def _():
                self.hop(s, way, shard, self.z + 1 - 2 * way).wait_recv()
                if s + 1 < self.fs:
                    nways = self.cases(s + 1)[way]

                    @pl.when(nways[1])
                    def _():
                        self.hop(s + 1, way, nways[2], nways[3]).start()
                self.swap(s, way, shard, self.y).start()

    def finish(self):
        self.own.wait()
        for s in range(1, self.fs):
            for way, sends, sent, device, gets, shard in self.cases(s):
                @pl.when(sends)
                def _():
                    self.hop(s, way, sent, device).wait_send()

                @pl.when(gets)
                def _():
                    self.swap(s, way, shard, self.y).wait_send()
                    self.swap(s, way, shard, 1 - self.y).wait_recv()


def along_scratch(fs):
    return [pltpu.SemaphoreType.DMA((4, 2, fs - 1)), pltpu.SemaphoreType.DMA]


def greet(tp, fs):
    me, z, y = lax.axis_index("tp"), lax.axis_index("fs"), lax.axis_index("grp")
    core, chip, chips = lax.rem(me, 2), me // 2, tp // 2
    barrier = pltpu.get_barrier_semaphore()
    devices = [{"tp": me + 1 - 2 * core}, {"grp": 1 - y}]
    devices += [{"tp": lax.rem(chip + d, chips) * 2 + core} for d in range(1, chips)]
    devices += [{"fs": lax.rem(z + d, fs)} for d in range(1, fs)]
    for device in devices:
        pl.semaphore_signal(barrier, inc=1, device_id=device, device_id_type=MESH)
    pl.semaphore_wait(barrier, len(devices))


def norm_rows(tp, held, gain, out):
    _, rows, columns = held.shape
    step = 128

    def body(i, carry):
        part = pl.ds(pl.multiple_of(i * step, step), step)
        total = jnp.zeros((step, 1), jnp.float32)
        for q in range(tp):
            values = held[q, part, :].astype(jnp.float32)
            total = total + jnp.sum(values * values, axis=-1, keepdims=True)
        inverse = lax.rsqrt(total / (tp * columns) + 1e-06)
        for q in range(tp):
            cols = slice(q * columns, (q + 1) * columns)
            values = held[q, part, :].astype(jnp.float32)
            out[part, cols] = (values * inverse * gain[:, cols]).astype(jnp.bfloat16)
        return carry

    lax.fori_loop(0, rows // step, body, 0)


def first_kernel(tp, fs, tokens, gain, mixer_src, scale_src, normed, mixers, scales, *scratch):
    across = Across(tp, tokens, *scratch[:7])
    along = Along(fs, mixer_src, mixers, *scratch[7:9])
    scale_sems, scale_local = scratch[9:]
    greet(tp, fs)
    z = lax.axis_index("fs")
    along.start()
    for k in range(CHUNKS):
        across.start_part(k)
    across.start_own()
    own = pltpu.make_async_copy(scale_src, scales.at[z], scale_local)
    own.start()
    small = []
    for d in range(1, fs):
        small.append(pltpu.make_async_remote_copy(
            src_ref=scale_src, dst_ref=scales.at[z], send_sem=scale_sems.at[0, d - 1],
            recv_sem=scale_sems.at[1, d - 1], device_id={"fs": lax.rem(z + d, fs)},
            device_id_type=MESH))
        small[-1].start()
    for k in range(CHUNKS):
        across.forward(k)
        if k + 1 < fs:
            along.pump(k + 1)
    for s in range(CHUNKS + 1, fs):
        along.pump(s)
    across.finish()
    norm_rows(tp, across.held, gain, normed)
    own.wait()
    for copy in small:
        copy.wait()
    along.finish()


ANY = pl.BlockSpec(memory_space=pl.ANY)


def first(tp, fs, tokens, gain, mixer_src, scale_src):
    rows, columns = tokens.shape
    return pl.pallas_call(
        functools.partial(first_kernel, tp, fs),
        out_shape=(
            jax.ShapeDtypeStruct((rows, columns * tp), jnp.bfloat16),
            jax.ShapeDtypeStruct((fs,) + mixer_src.shape, jnp.bfloat16),
            jax.ShapeDtypeStruct((fs,) + scale_src.shape, jnp.float32),
        ),
        in_specs=[VMEM] * 4, out_specs=(VMEM, ANY, VMEM),
        scratch_shapes=across_scratch(tp, rows, columns) + along_scratch(fs) + [
            pltpu.SemaphoreType.DMA((2, fs - 1)), pltpu.SemaphoreType.DMA],
        compiler_params=pltpu.CompilerParams(
            collective_id=0, has_side_effects=True, vmem_limit_bytes=40 * 2**20),
        cost_estimate=pl.CostEstimate(flops=10**7, bytes_accessed=60 * 2**20, transcendentals=0),
        name="first",
    )(tokens, gain[None], mixer_src, scale_src)


def second_kernel(
    tp, fs, state, weight, scale, tokens, gain, val_src, down_src, hidden, normed, val_out,
    down_out, *scratch,
):
    states = Across(tp, state, *scratch[:7])
    hiddens = Across(tp, hidden, *scratch[7:14])
    val = Along(fs, val_src, val_out, *scratch[14:16])
    down = Along(fs, down_src, down_out, *scratch[16:18])
    greet(tp, fs)
    val.start()
    for k in range(CHUNKS):
        states.start_part(k)
    states.start_own()
    down.start()
    for k in range(CHUNKS):
        states.forward(k)
    states.finish()
    held, columns = states.held, state.shape[1]
    step = tokens.shape[0] // CHUNKS
    for k in range(CHUNKS):
        part = pl.ds(k * step, step)
        mixed = jnp.zeros((step, tokens.shape[1]), jnp.float32)
        for q in range(tp):
            term = jnp.dot(
                held[q, part, :], weight[q * columns : (q + 1) * columns, :],
                preferred_element_type=jnp.float32) * scale[...]
            mixed = mixed + term.astype(jnp.bfloat16).astype(jnp.float32)
        hidden[part, :] = (tokens[part, :].astype(jnp.float32) + mixed).astype(jnp.bfloat16)
        hiddens.start_part(k)
    hiddens.start_own()
    val.pump(1)
    hiddens.forward(0)
    hiddens.forward(1)
    down.pump(1)
    for k in range(2, CHUNKS):
        hiddens.forward(k)
    if fs > 2:
        val.pump(2)
    hiddens.finish()
    norm_rows(tp, hiddens.held, gain, normed)
    if fs > 2:
        down.pump(2)
    for s in range(3, fs):
        val.pump(s)
        down.pump(s)
    val.finish()
    down.finish()


def second(tp, fs, state, weight, scale, tokens, gain, val_src, down_src):
    rows, columns = tokens.shape
    return pl.pallas_call(
        functools.partial(second_kernel, tp, fs),
        out_shape=(
            jax.ShapeDtypeStruct((rows, columns), jnp.bfloat16),
            jax.ShapeDtypeStruct((rows, columns * tp), jnp.bfloat16),
            jax.ShapeDtypeStruct((fs,) + val_src.shape, jnp.bfloat16),
            jax.ShapeDtypeStruct((fs,) + down_src.shape, jnp.bfloat16),
        ),
        in_specs=[VMEM] * 7, out_specs=(VMEM, VMEM, ANY, ANY),
        scratch_shapes=across_scratch(tp, rows, state.shape[1]) + across_scratch(tp, rows, columns)
        + along_scratch(fs) + along_scratch(fs),
        compiler_params=pltpu.CompilerParams(
            collective_id=1, has_side_effects=True, vmem_limit_bytes=48 * 2**20),
        cost_estimate=pl.CostEstimate(flops=10**9, bytes_accessed=180 * 2**20, transcendentals=0),
        name="second",
    )(state, weight, scale[None], tokens, gain[None], val_src, down_src)


def half_rows(weight):
    count = lax.axis_size("grp")
    rows = weight.shape[0] // count
    start = lax.axis_index("grp") * rows
    return lax.dynamic_slice_in_dim(weight, start, rows, 0).astype(jnp.bfloat16)


def whole_rows(weight):
    return lax.all_gather(half_rows(weight), ("fs", "grp"), axis=0, tiled=True)


def halves(weight):
    count = lax.axis_size("grp")
    return weight.astype(jnp.bfloat16).reshape(count, weight.shape[0] // count, weight.shape[1])


def per_device(
    tokens, mixer_gain, branch_weight, gelu_weight, branch_scale, gelu_scale, branch_taps,
    recur_gate, input_gate, decay_param, out_weight, out_scale, ffn_gain, upgate_weight,
    upval_weight, upgate_scale, upval_scale, upgate_taps, upval_taps, down_weight, down_scale,
):
    tp = lax.axis_size("tp")
    fs = lax.axis_size("fs")
    gate_full = whole_rows(upgate_weight)
    scale_list = (branch_scale, gelu_scale, out_scale, upgate_scale, upval_scale, down_scale)
    lru = branch_weight.shape[1]
    depth = branch_weight.shape[0] // 2
    mixer_src = jnp.concatenate(
        [halves(branch_weight), halves(gelu_weight), halves(out_weight.reshape(-1, lru))], axis=1)
    normed, mixers, packed = first(
        tp, fs, tokens, mixer_gain, mixer_src, jnp.concatenate(scale_list, axis=1))
    packed = packed[:, 0]
    scales, start = [], 0
    for piece in scale_list:
        scales.append(expand_scale(packed[:, start : start + piece.shape[1]]))
        start += piece.shape[1]
    rows_branch = mixers[:, :, :depth].reshape(-1, lru)
    rows_gelu = mixers[:, :, depth : 2 * depth].reshape(-1, lru)
    out_blocks = mixers[:, :, 2 * depth :].reshape((fs,) + out_weight.shape)
    branch = jnp.dot(normed, rows_branch, preferred_element_type=jnp.float32)
    gelu_in = jnp.dot(normed, rows_gelu, preferred_element_type=jnp.float32)
    gated_state = mixer(
        branch, gelu_in, scales[0], scales[1], branch_taps, recur_gate, input_gate,
        jax.nn.softplus(-decay_param))
    row_block = jnp.transpose(out_blocks, (1, 0, 2)).reshape(out_weight.shape[0], -1)
    own_columns = lax.all_to_all(row_block, "tp", split_axis=1, concat_axis=0, tiled=True)
    width = tokens.shape[1]
    own_scales = lax.dynamic_slice_in_dim(scales[2], lax.axis_index("tp") * width, width, 0)
    hidden_state, normed_ffn, value_full, down_blocks = second(
        tp, fs, gated_state, own_columns, own_scales, tokens, ffn_gain,
        halves(upval_weight), halves(down_weight))
    value_full = value_full.reshape(-1, upval_weight.shape[1])
    down_blocks = down_blocks.reshape((fs,) + down_weight.shape)
    up_gate = jnp.dot(normed_ffn, gate_full, preferred_element_type=jnp.float32)
    up_val = jnp.dot(normed_ffn, value_full, preferred_element_type=jnp.float32)
    conv_gate = causal_mix(up_gate * scales[3], upgate_taps, SEQ_LEN)
    conv_val = causal_mix(up_val * scales[4], upval_taps, SEQ_LEN)
    ffn_hidden = (jax.nn.silu(conv_gate) * conv_val).astype(jnp.bfloat16)
    piece = down_blocks.shape[2]
    terms = []
    for f in range(down_blocks.shape[0]):
        term = jnp.dot(ffn_hidden, down_blocks[f], preferred_element_type=jnp.float32)
        terms.append((term * scales[5][f * piece : (f + 1) * piece]).astype(jnp.bfloat16))
    ffn_terms = jnp.concatenate(terms, axis=1)
    ffn_sum = lax.psum_scatter(ffn_terms, "tp", scatter_dimension=1, tiled=True).astype(jnp.float32)
    return (hidden_state.astype(jnp.float32) + ffn_sum).astype(jnp.bfloat16)


def solution(mesh):
    in_specs = (
        P(("grp", "fs"), "tp"), P(), P("fs", "tp"), P("fs", "tp"), P("fs", "tp"), P("fs", "tp"),
        P(None, "tp"), P("tp", None, None), P("tp", None, None), P("tp"), P("tp", "fs"),
        P("fs", None), P(), P("fs", "tp"), P("fs", "tp"), P("fs", "tp"), P("fs", "tp"),
        P(None, "tp"), P(None, "tp"), P("tp", "fs"), P("fs", None),
    )
    return jax.shard_map(
        per_device, mesh=mesh, in_specs=in_specs, out_specs=P(("grp", "fs"), "tp"), check_vma=False
    )
```

```python
import functools

import jax
import jax.numpy as jnp
from jax import lax
from jax.experimental import pallas as pl
from jax.experimental.pallas import tpu as pltpu
from jax.sharding import PartitionSpec as P

SEQ_LEN = 512
MESH = pl.DeviceIdType.MESH
VMEM = pl.BlockSpec(memory_space=pltpu.VMEM)
CHUNKS = 4


def expand_scale(gathered):
    return gathered.T.reshape(-1)


def mixer_kernel(branch_ref, gelu_ref, bscale_ref, gscale_ref, taps_ref, rg_ref, ig_ref, sp_ref, out_ref):
    branch = branch_ref[...] * bscale_ref[...]
    rows = branch.shape[0]
    position = lax.broadcasted_iota(jnp.int32, branch.shape, 0)

    def delayed(values, shift, fill):
        return jnp.where(position >= shift, pltpu.roll(values, shift, 0), fill)

    taps = taps_ref.shape[0]
    conv = branch * taps_ref[taps - 1 : taps, :]
    for k in range(taps - 1):
        conv = conv + delayed(branch, taps - 1 - k, 0.0) * taps_ref[k : k + 1, :]
    conv_bf = conv.astype(jnp.bfloat16)
    conv = conv_bf.astype(jnp.float32)
    recur = jax.nn.sigmoid(jnp.dot(conv_bf, rg_ref[...], preferred_element_type=jnp.float32))
    rate = jax.nn.sigmoid(jnp.dot(conv_bf, ig_ref[...], preferred_element_type=jnp.float32))
    log_decay = -8.0 * recur * sp_ref[...]
    factor = jnp.exp(log_decay)
    state = jnp.sqrt(-jnp.tanh(log_decay) * (factor * factor + 1.0)) * rate * conv
    shift = 1
    while shift < rows:
        state = factor * delayed(state, shift, 0.0) + state
        factor = factor * delayed(factor, shift, 1.0)
        shift *= 2
    gelu_in = gelu_ref[...] * gscale_ref[...]
    out_ref[...] = (state * jax.nn.gelu(gelu_in)).astype(jnp.bfloat16)


def block_diagonal(gate, per):
    count, width, _ = gate.shape
    grouped = gate.reshape(count // per, per, width, width)
    eye = jnp.eye(per, dtype=gate.dtype)
    return jnp.einsum("gpab,pq->gpaqb", grouped, eye).reshape(count // per, per * width, per * width)


def mixer(branch, gelu_in, flat, branch_start, gelu_start, taps, recur_gate, input_gate, softplus):
    rows, channels = branch.shape
    lanes = min(channels, 128)
    per = lanes // recur_gate.shape[1]
    rg, ig = block_diagonal(recur_gate, per), block_diagonal(input_gate, per)
    tile = pl.BlockSpec((SEQ_LEN, lanes), lambda s, c: (s, c))
    row = pl.BlockSpec((1, lanes), lambda s, c: (0, c))
    bscale, boff = aligned(flat, branch_start, channels)
    gscale, goff = aligned(flat, gelu_start, channels)
    gate = pl.BlockSpec((None, lanes, lanes), lambda s, c: (c, 0, 0))
    return pl.pallas_call(
        mixer_kernel,
        grid=(rows // SEQ_LEN, channels // lanes),
        out_shape=jax.ShapeDtypeStruct((rows, channels), jnp.bfloat16),
        in_specs=[
            tile, tile,
            pl.BlockSpec((1, lanes), lambda s, c: (0, c + boff)),
            pl.BlockSpec((1, lanes), lambda s, c: (0, c + goff)),
            pl.BlockSpec((taps.shape[0], lanes), lambda s, c: (0, c)),
            gate, gate, row,
        ],
        out_specs=tile,
        cost_estimate=pl.CostEstimate(flops=10**8, bytes_accessed=10 * rows * channels, transcendentals=rows * channels * 6),
    )(branch, gelu_in, bscale, gscale, taps, rg, ig, softplus[None])


class Across:
    def __init__(self, tp, src, held, local_sem, pair_sems, sends, recvs, fsends, frecvs):
        self.src, self.held, self.local_sem, self.pair_sems = src, held, local_sem, pair_sems
        self.sems = (sends, recvs, fsends, frecvs)
        self.me = lax.axis_index("tp")
        self.core, self.chips = lax.rem(self.me, 2), tp // 2
        self.chip = self.me // 2
        self.partner = self.me + 1 - 2 * self.core
        self.rows = src.shape[0] // CHUNKS
        self.others = [
            lax.rem(self.chip + d, self.chips) * 2 + self.core for d in range(1, self.chips)]
        self.open = []

    def copy(self, source, dest, send, recv, device):
        return pltpu.make_async_remote_copy(
            src_ref=source, dst_ref=dest, send_sem=send, recv_sem=recv,
            device_id={"tp": device}, device_id_type=MESH)

    def start_part(self, k):
        part = pl.ds(k * self.rows, self.rows)
        for d in range(1, self.chips):
            copy = self.copy(
                self.src.at[part], self.held.at[self.me, part], self.sems[0].at[d - 1, k],
                self.sems[1].at[d - 1, k], self.others[d - 1])
            copy.start()
            self.open.append(copy.wait_send)

    def start_own(self):
        own = pltpu.make_async_copy(self.src, self.held.at[self.me], self.local_sem)
        own.start()
        pair = self.copy(
            self.src, self.held.at[self.me], self.pair_sems.at[0], self.pair_sems.at[1],
            self.partner)
        pair.start()
        self.open += [own.wait, pair.wait]

    def forward(self, k):
        part = pl.ds(k * self.rows, self.rows)
        for d in range(1, self.chips):
            source = lax.rem(self.chip - d + self.chips, self.chips) * 2 + self.core
            self.copy(
                self.src.at[part], self.held.at[source, part], self.sems[0].at[d - 1, k],
                self.sems[1].at[d - 1, k], self.others[d - 1]).wait_recv()
            onward = self.copy(
                self.held.at[source, part], self.held.at[source, part],
                self.sems[2].at[d - 1, k], self.sems[3].at[d - 1, k], self.partner)
            onward.start()
            self.open.append(onward.wait)

    def finish(self):
        for wait in self.open:
            wait()


def across_scratch(tp, rows, columns):
    many = pltpu.SemaphoreType.DMA((tp // 2 - 1, CHUNKS))
    return [
        pltpu.VMEM((tp, rows, columns), jnp.bfloat16),
        pltpu.SemaphoreType.DMA, pltpu.SemaphoreType.DMA((2,)), many, many, many, many,
    ]


class Along:
    def __init__(self, fs, src, out, sems, local_sem):
        self.fs, self.src, self.out, self.sems, self.local_sem = fs, src, out, sems, local_sem
        self.z, self.y = lax.axis_index("fs"), lax.axis_index("grp")

    def cases(self, s):
        z, fs = self.z, self.fs
        return (
            (0, (z >= s - 1) & (z <= fs - 2), z - s + 1, z + 1, z >= s, z - s),
            (1, (z >= 1) & (z <= fs - s), z + s - 1, z - 1, z <= fs - 1 - s, z + s),
        )

    def hop(self, s, way, shard, device):
        source = self.src.at[self.y] if s == 1 else self.out.at[shard, self.y]
        return pltpu.make_async_remote_copy(
            src_ref=source, dst_ref=self.out.at[shard, self.y],
            send_sem=self.sems.at[0, way, s - 1], recv_sem=self.sems.at[1, way, s - 1],
            device_id={"fs": device}, device_id_type=MESH)

    def swap(self, s, way, shard, half):
        where = self.out.at[shard, half]
        return pltpu.make_async_remote_copy(
            src_ref=where, dst_ref=where,
            send_sem=self.sems.at[2, way, s - 1], recv_sem=self.sems.at[3, way, s - 1],
            device_id={"grp": 1 - self.y}, device_id_type=MESH)

    def start(self):
        self.own = pltpu.make_async_copy(self.src, self.out.at[self.z], self.local_sem)
        self.send(1)
        self.own.start()

    def send(self, s):
        for way, sends, shard, device, _, _ in self.cases(s):
            @pl.when(sends)
            def _():
                self.hop(s, way, shard, device).start()

    def pump(self, s):
        for way, _, _, _, gets, shard in self.cases(s):
            @pl.when(gets)
            def _():
                self.hop(s, way, shard, self.z + 1 - 2 * way).wait_recv()
                if s + 1 < self.fs:
                    nways = self.cases(s + 1)[way]

                    @pl.when(nways[1])
                    def _():
                        self.hop(s + 1, way, nways[2], nways[3]).start()
                self.swap(s, way, shard, self.y).start()

    def finish(self):
        self.own.wait()
        for s in range(1, self.fs):
            for way, sends, sent, device, gets, shard in self.cases(s):
                @pl.when(sends)
                def _():
                    self.hop(s, way, sent, device).wait_send()

                @pl.when(gets)
                def _():
                    self.swap(s, way, shard, self.y).wait_send()
                    self.swap(s, way, shard, 1 - self.y).wait_recv()


def along_scratch(fs):
    return [pltpu.SemaphoreType.DMA((4, 2, fs - 1)), pltpu.SemaphoreType.DMA]


def greet(tp, fs):
    me, z, y = lax.axis_index("tp"), lax.axis_index("fs"), lax.axis_index("grp")
    core, chip, chips = lax.rem(me, 2), me // 2, tp // 2
    barrier = pltpu.get_barrier_semaphore()
    devices = [{"tp": me + 1 - 2 * core}, {"grp": 1 - y}]
    devices += [{"tp": lax.rem(chip + d, chips) * 2 + core} for d in range(1, chips)]
    devices += [{"fs": lax.rem(z + d, fs)} for d in range(1, fs)]
    for device in devices:
        pl.semaphore_signal(barrier, inc=1, device_id=device, device_id_type=MESH)
    pl.semaphore_wait(barrier, len(devices))


def norm_rows(tp, held, gain, out):
    _, rows, columns = held.shape
    step = 128

    def body(i, carry):
        part = pl.ds(pl.multiple_of(i * step, step), step)
        total = jnp.zeros((step, 1), jnp.float32)
        for q in range(tp):
            values = held[q, part, :].astype(jnp.float32)
            total = total + jnp.sum(values * values, axis=-1, keepdims=True)
        inverse = lax.rsqrt(total / (tp * columns) + 1e-06)
        for q in range(tp):
            cols = slice(q * columns, (q + 1) * columns)
            values = held[q, part, :].astype(jnp.float32)
            out[part, cols] = (values * inverse * gain[:, cols]).astype(jnp.bfloat16)
        return carry

    lax.fori_loop(0, rows // step, body, 0)


def first_kernel(
    tp, fs, tokens, gain, mixer_src, scale_src, gate_src, normed, mixers, scales, gate_out, *scratch
):
    across = Across(tp, tokens, *scratch[:7])
    along = Along(fs, mixer_src, mixers, *scratch[7:9])
    scale_sems, scale_local = scratch[9:11]
    gate = Along(fs, gate_src, gate_out, *scratch[11:13])
    greet(tp, fs)
    z = lax.axis_index("fs")
    along.start()
    for k in range(CHUNKS):
        across.start_part(k)
    across.start_own()
    own = pltpu.make_async_copy(scale_src, scales.at[z], scale_local)
    own.start()
    small = []
    for d in range(1, fs):
        small.append(pltpu.make_async_remote_copy(
            src_ref=scale_src, dst_ref=scales.at[z], send_sem=scale_sems.at[0, d - 1],
            recv_sem=scale_sems.at[1, d - 1], device_id={"fs": lax.rem(z + d, fs)},
            device_id_type=MESH))
        small[-1].start()
    gate.start()
    for k in range(CHUNKS):
        across.forward(k)
        if k + 1 < fs:
            along.pump(k + 1)
    for s in range(CHUNKS + 1, fs):
        along.pump(s)
    gate.pump(1)
    across.finish()
    norm_rows(tp, across.held, gain, normed)
    own.wait()
    for s in range(2, fs):
        gate.pump(s)
    gate.finish()
    for copy in small:
        copy.wait()
    along.finish()


ANY = pl.BlockSpec(memory_space=pl.ANY)


def first(tp, fs, tokens, gain, mixer_src, scale_src, gate_src):
    rows, columns = tokens.shape
    return pl.pallas_call(
        functools.partial(first_kernel, tp, fs),
        out_shape=(
            jax.ShapeDtypeStruct((rows, columns * tp), jnp.bfloat16),
            jax.ShapeDtypeStruct((fs,) + mixer_src.shape, jnp.bfloat16),
            jax.ShapeDtypeStruct((fs,) + scale_src.shape, jnp.float32),
            jax.ShapeDtypeStruct((fs,) + gate_src.shape, jnp.bfloat16),
        ),
        in_specs=[VMEM] * 5, out_specs=(VMEM, ANY, VMEM, ANY),
        scratch_shapes=across_scratch(tp, rows, columns) + along_scratch(fs) + [
            pltpu.SemaphoreType.DMA((2, fs - 1)), pltpu.SemaphoreType.DMA] + along_scratch(fs),
        compiler_params=pltpu.CompilerParams(
            collective_id=0, has_side_effects=True, vmem_limit_bytes=40 * 2**20),
        cost_estimate=pl.CostEstimate(flops=10**7, bytes_accessed=60 * 2**20, transcendentals=0),
        name="first",
    )(tokens, gain[None], mixer_src, scale_src, gate_src)


def second_kernel(
    tp, fs, state, weight, scale, tokens, gain, val_src, down_src, hidden, normed, val_out,
    down_out, *scratch,
):
    states = Across(tp, state, *scratch[:7])
    hiddens = Across(tp, hidden, *scratch[7:14])
    val = Along(fs, val_src, val_out, *scratch[14:16])
    down = Along(fs, down_src, down_out, *scratch[16:18])
    greet(tp, fs)
    val.start()
    for k in range(CHUNKS):
        states.start_part(k)
    states.start_own()
    down.start()
    for k in range(CHUNKS):
        states.forward(k)
    states.finish()
    held, columns = states.held, state.shape[1]
    step = tokens.shape[0] // CHUNKS
    for k in range(CHUNKS):
        part = pl.ds(k * step, step)
        mixed = jnp.zeros((step, tokens.shape[1]), jnp.float32)
        for q in range(tp):
            term = jnp.dot(
                held[q, part, :], weight[q * columns : (q + 1) * columns, :],
                preferred_element_type=jnp.float32) * scale[...]
            mixed = mixed + term.astype(jnp.bfloat16).astype(jnp.float32)
        hidden[part, :] = (tokens[part, :].astype(jnp.float32) + mixed).astype(jnp.bfloat16)
        hiddens.start_part(k)
    hiddens.start_own()
    val.pump(1)
    hiddens.forward(0)
    hiddens.forward(1)
    down.pump(1)
    for k in range(2, CHUNKS):
        hiddens.forward(k)
    if fs > 2:
        val.pump(2)
    hiddens.finish()
    norm_rows(tp, hiddens.held, gain, normed)
    if fs > 2:
        down.pump(2)
    for s in range(3, fs):
        val.pump(s)
        down.pump(s)
    val.finish()
    down.finish()


def second(tp, fs, state, weight, scale, tokens, gain, val_src, down_src):
    rows, columns = tokens.shape
    return pl.pallas_call(
        functools.partial(second_kernel, tp, fs),
        out_shape=(
            jax.ShapeDtypeStruct((rows, columns), jnp.bfloat16),
            jax.ShapeDtypeStruct((rows, columns * tp), jnp.bfloat16),
            jax.ShapeDtypeStruct((fs,) + val_src.shape, jnp.bfloat16),
            jax.ShapeDtypeStruct((fs,) + down_src.shape, jnp.bfloat16),
        ),
        in_specs=[VMEM] * 7, out_specs=(VMEM, VMEM, ANY, ANY),
        scratch_shapes=across_scratch(tp, rows, state.shape[1]) + across_scratch(tp, rows, columns)
        + along_scratch(fs) + along_scratch(fs),
        compiler_params=pltpu.CompilerParams(
            collective_id=1, has_side_effects=True, vmem_limit_bytes=48 * 2**20),
        cost_estimate=pl.CostEstimate(flops=10**9, bytes_accessed=180 * 2**20, transcendentals=0),
        name="second",
    )(state, weight, scale[None], tokens, gain[None], val_src, down_src)


def last_kernel(
    tp, left, down, scale, hidden, out, terms, near, pairs, far, kept,
    near_send, near_recv, far_send, far_recv,
):
    me = lax.axis_index("tp")
    core, chip, chips = lax.rem(me, 2), me // 2, tp // 2
    partner = me + 1 - 2 * core
    others = [lax.rem(chip + d, chips) for d in range(chips)]
    barrier = pltpu.get_barrier_semaphore()
    for device in [partner] + [c * 2 + core for c in others[1:]]:
        pl.semaphore_signal(barrier, inc=1, device_id={"tp": device}, device_id_type=MESH)
    pl.semaphore_wait(barrier, chips)
    rows = left.shape[0] // CHUNKS
    per = down.shape[0] // tp
    piece = down.shape[2]

    def term(k, block):
        values = left[k * rows : (k + 1) * rows, :]
        cols = [
            jnp.dot(values, down[block * per + j], preferred_element_type=jnp.float32)
            for j in range(per)]
        whole = cols[0] if per == 1 else jnp.concatenate(cols, axis=1)
        return (whole * scale[block]).astype(jnp.bfloat16)

    def to_partner(k, c):
        return pltpu.make_async_remote_copy(
            src_ref=terms.at[k, 0, c], dst_ref=near.at[k, c], send_sem=near_send.at[k, c],
            recv_sem=near_recv.at[k, c], device_id={"tp": partner}, device_id_type=MESH)

    def to_chip(k, d):
        return pltpu.make_async_remote_copy(
            src_ref=pairs.at[k, d - 1], dst_ref=far.at[k, d - 1], send_sem=far_send.at[k, d - 1],
            recv_sem=far_recv.at[k, d - 1], device_id={"tp": others[d] * 2 + core},
            device_id_type=MESH)

    def join(k):
        for d in list(range(1, chips)) + [0]:
            c = others[d]
            to_partner(k, c).wait_recv()
            total = terms[k, 1, c].astype(jnp.float32) + near[k, c].astype(jnp.float32)
            if d:
                pairs[k, d - 1] = total.astype(jnp.bfloat16)
                to_chip(k, d).start()
            else:
                kept[k] = total

    def close(k):
        total = kept[k]
        for d in range(1, chips):
            to_chip(k, d).wait_recv()
            total = total + far[k, d - 1].astype(jnp.float32)
        part = slice(k * rows, (k + 1) * rows)
        out[part, :] = (hidden[part, :].astype(jnp.float32) + total).astype(jnp.bfloat16)

    for k in range(CHUNKS):
        for d in list(range(1, chips)) + [0]:
            c = others[d]
            terms[k, 0, c] = term(k, c * 2 + 1 - core)
            to_partner(k, c).start()
        for d in list(range(1, chips)) + [0]:
            c = others[d]
            terms[k, 1, c] = term(k, c * 2 + core)
        join(k)
    for k in range(CHUNKS):
        close(k)
    for k in range(CHUNKS):
        for c in others:
            to_partner(k, c).wait_send()
        for d in range(1, chips):
            to_chip(k, d).wait_send()


def last(tp, left, down, scale, hidden):
    rows, width = hidden.shape
    chips, part = tp // 2, rows // CHUNKS
    return pl.pallas_call(
        functools.partial(last_kernel, tp),
        out_shape=jax.ShapeDtypeStruct(hidden.shape, jnp.bfloat16),
        in_specs=[VMEM] * 4, out_specs=VMEM,
        scratch_shapes=[
            pltpu.VMEM((CHUNKS, 2, chips, part, width), jnp.bfloat16),
            pltpu.VMEM((CHUNKS, chips, part, width), jnp.bfloat16),
            pltpu.VMEM((CHUNKS, chips - 1, part, width), jnp.bfloat16),
            pltpu.VMEM((CHUNKS, chips - 1, part, width), jnp.bfloat16),
            pltpu.VMEM((CHUNKS, part, width), jnp.float32),
            pltpu.SemaphoreType.DMA((CHUNKS, chips)), pltpu.SemaphoreType.DMA((CHUNKS, chips)),
            pltpu.SemaphoreType.DMA((CHUNKS, chips - 1)),
            pltpu.SemaphoreType.DMA((CHUNKS, chips - 1)),
        ],
        compiler_params=pltpu.CompilerParams(
            collective_id=2, has_side_effects=True, vmem_limit_bytes=48 * 2**20),
        cost_estimate=pl.CostEstimate(flops=10**10, bytes_accessed=60 * 2**20, transcendentals=0),
        name="last",
    )(left, down, scale.reshape(tp, 1, width), hidden)


def aligned(flat, start, size):
    if start % 128 == 0:
        return flat, start // 128
    return flat[:, start : start + size], 0


def up_kernel(left_ref, gate_ref, val_ref, gscale_ref, vscale_ref, gtaps_ref, vtaps_ref, out_ref):
    lanes = gate_ref.shape[1]
    weight = jnp.concatenate([gate_ref[...], val_ref[...]], axis=1)

    def mixed(values, scale_ref, taps_ref):
        values = values * scale_ref[...]
        position = lax.broadcasted_iota(jnp.int32, values.shape, 0)
        taps = taps_ref.shape[0]
        total = values * taps_ref[taps - 1 : taps, :]
        for shift in range(1, taps):
            delayed = jnp.where(position >= shift, pltpu.roll(values, shift, 0), 0.0)
            total = total + delayed * taps_ref[taps - 1 - shift : taps - shift, :]
        return total

    for s in range(left_ref.shape[0] // SEQ_LEN):
        part = slice(s * SEQ_LEN, (s + 1) * SEQ_LEN)
        both = jnp.dot(left_ref[part, :], weight, preferred_element_type=jnp.float32)
        gate = mixed(both[:, :lanes], gscale_ref, gtaps_ref)
        value = mixed(both[:, lanes:], vscale_ref, vtaps_ref)
        out_ref[part, :] = (jax.nn.silu(gate) * value).astype(jnp.bfloat16)


def up(left, gate, val, flat, gate_start, val_start, gate_taps, val_taps):
    rows, depth = left.shape
    columns = gate.shape[1]
    lanes = 128
    gscale, goff = aligned(flat, gate_start, columns)
    vscale, voff = aligned(flat, val_start, columns)
    tile = pl.BlockSpec((depth, lanes), lambda c: (0, c))
    tap = pl.BlockSpec((gate_taps.shape[0], lanes), lambda c: (0, c))
    return pl.pallas_call(
        up_kernel,
        grid=(pl.cdiv(columns, lanes),),
        out_shape=jax.ShapeDtypeStruct((rows, columns), jnp.bfloat16),
        in_specs=[
            pl.BlockSpec((rows, depth), lambda c: (0, 0)), tile, tile,
            pl.BlockSpec((1, lanes), lambda c: (0, c + goff)),
            pl.BlockSpec((1, lanes), lambda c: (0, c + voff)), tap, tap,
        ],
        out_specs=pl.BlockSpec((rows, lanes), lambda c: (0, c)),
        compiler_params=pltpu.CompilerParams(vmem_limit_bytes=32 * 2**20),
        cost_estimate=pl.CostEstimate(
            flops=4 * rows * depth * columns, bytes_accessed=20 * 2**20, transcendentals=rows * columns),
        name="up",
    )(left, gate, val, gscale, vscale, gate_taps, val_taps)


def half_rows(weight):
    count = lax.axis_size("grp")
    rows = weight.shape[0] // count
    start = lax.axis_index("grp") * rows
    return lax.dynamic_slice_in_dim(weight, start, rows, 0).astype(jnp.bfloat16)


def whole_rows(weight):
    return lax.all_gather(half_rows(weight), ("fs", "grp"), axis=0, tiled=True)


def halves(weight):
    count = lax.axis_size("grp")
    return weight.astype(jnp.bfloat16).reshape(count, weight.shape[0] // count, weight.shape[1])


def per_device(
    tokens, mixer_gain, branch_weight, gelu_weight, branch_scale, gelu_scale, branch_taps,
    recur_gate, input_gate, decay_param, out_weight, out_scale, ffn_gain, upgate_weight,
    upval_weight, upgate_scale, upval_scale, upgate_taps, upval_taps, down_weight, down_scale,
):
    tp = lax.axis_size("tp")
    fs = lax.axis_size("fs")
    scale_list = (branch_scale, gelu_scale, out_scale, upgate_scale, upval_scale, down_scale)
    lru = branch_weight.shape[1]
    depth = branch_weight.shape[0] // 2
    mixer_src = jnp.concatenate(
        [halves(branch_weight), halves(gelu_weight), halves(out_weight.reshape(-1, lru))], axis=1)
    normed, mixers, packed, gate_full = first(
        tp, fs, tokens, mixer_gain, mixer_src, jnp.concatenate(scale_list, axis=1),
        halves(upgate_weight))
    gate_full = gate_full.reshape(-1, upgate_weight.shape[1])
    flat = expand_scale(packed[:, 0])[None]
    starts = [0]
    for piece in scale_list:
        starts.append(starts[-1] + piece.shape[1] * fs)
    rows_branch = mixers[:, :, :depth].reshape(-1, lru)
    rows_gelu = mixers[:, :, depth : 2 * depth].reshape(-1, lru)
    out_blocks = mixers[:, :, 2 * depth :].reshape((fs,) + out_weight.shape)
    branch = jnp.dot(normed, rows_branch, preferred_element_type=jnp.float32)
    gelu_in = jnp.dot(normed, rows_gelu, preferred_element_type=jnp.float32)
    gated_state = mixer(
        branch, gelu_in, flat, starts[0], starts[1], branch_taps, recur_gate, input_gate,
        jax.nn.softplus(-decay_param))
    row_block = jnp.transpose(out_blocks, (1, 0, 2)).reshape(out_weight.shape[0], -1)
    own_columns = lax.all_to_all(row_block, "tp", split_axis=1, concat_axis=0, tiled=True)
    width = tokens.shape[1]
    own_scales = lax.dynamic_slice_in_dim(
        flat[0], starts[2] + lax.axis_index("tp") * width, width, 0)
    hidden_state, normed_ffn, value_full, down_blocks = second(
        tp, fs, gated_state, own_columns, own_scales, tokens, ffn_gain,
        halves(upval_weight), halves(down_weight))
    value_full = value_full.reshape(-1, upval_weight.shape[1])
    down_blocks = down_blocks.reshape((fs,) + down_weight.shape)
    ffn_hidden = up(
        normed_ffn, gate_full, value_full, flat, starts[3], starts[4], upgate_taps, upval_taps)
    down_scales = flat[0, starts[5] : starts[5] + down_scale.shape[1] * fs]
    return last(tp, ffn_hidden, down_blocks, down_scales, hidden_state)


def solution(mesh):
    in_specs = (
        P(("grp", "fs"), "tp"), P(), P("fs", "tp"), P("fs", "tp"), P("fs", "tp"), P("fs", "tp"),
        P(None, "tp"), P("tp", None, None), P("tp", None, None), P("tp"), P("tp", "fs"),
        P("fs", None), P(), P("fs", "tp"), P("fs", "tp"), P("fs", "tp"), P("fs", "tp"),
        P(None, "tp"), P(None, "tp"), P("tp", "fs"), P("fs", None),
    )
    return jax.shard_map(
        per_device, mesh=mesh, in_specs=in_specs, out_specs=P(("grp", "fs"), "tp"), check_vma=False
    )
```
